32 devices in a mesh: ep: 8 (over z, y), tp: 4 (over x, core).
Axes of the slice: x: 2, y: 2, z: 4, core: 2. Of those that a mesh axis runs over, the one named last changes fastest.
Arguments:
- tokens: bfloat16 [2048, 2048], P('ep'), may hold values from -6 to 6
- norm_gain: float32 [2048], replicated, may hold values from 0.1 to 1.9
- expert_ids: int32 [2048, 2], P('ep'), may hold values from 0 to 3, all different within a row; in each aligned block of 256 rows (0 to 255, 256 to 511, ...) at most 160 rows name the same one
- route_weight: float32 [2048, 2], P('ep'), may hold values from 0.2 to 1
- w_gate: bfloat16 [8, 2048, 3584], P('ep', None, 'tp'), may hold values from -0.125 to 0.125
- w_up: bfloat16 [8, 2048, 3584], P('ep', None, 'tp'), may hold values from -0.125 to 0.125
- w_down: bfloat16 [8, 3584, 2048], P('ep', 'tp'), may hold values from -0.0625 to 0.0625
Outputs:
- mixed: bfloat16 [2048, 2048], P('ep', 'tp')
The draws below stay inside these ranges and needn't reach their ends.
Inputs may be any that keep to these rules, and one draw needn't show every extreme that they name: `expert_ids`: A token names 2 different experts. In each aligned block of 256 tokens (the tokens of one index of ep) no expert is named by more than 160 tokens, a bound that some block reaches.
All inputs are finite; a program needn't handle non-finite values.
Results may differ from the reference program's by a relative error of at most 0.014.
Values may be sent and summed in bfloat16 or wider, within the bound.
A program may use at most 128 MiB of HBM per device.

```python
import math
import jax
import jax.numpy as jnp
import numpy as np
from jax import lax

D = 2048
FF = 7168
TOP = 2
HALVES = 2
TOK_DEV = 256
EXPERTS = 4
HALF_FF = 3584
BLOCK_H = 896
CAP = 160
TOKENS = 2048
N_EP = 8
N_TP = 4


def steps_of(key, dims, pieces, smallest, top_value):
    loudness = 1.0
    for axis_at, shards_of in pieces:
        heights = jax.random.uniform(jax.random.fold_in(jax.random.fold_in(key, 6), axis_at), (shards_of,), jnp.float32, smallest / len(pieces), top_value / len(pieces))
        loudness = loudness * jnp.repeat(jnp.exp(heights), dims[axis_at] // shards_of).reshape((-1,) + (1,) * (len(dims) - 1 - axis_at))
    return loudness


def assign_block(rng, own, number, rows, number_of, top, bound, slope):
    sequence = jax.random.permutation(rng, number_of)
    packed, ordinary = shares(number_of, rows * top, bound, slope, True), shares(number_of, rows * top, bound, slope, False)
    places = jnp.arange(number_of)

    def named(tallies, offset_by):
        used = int((tallies > 0).sum())
        fixed = max(1, used // 4)
        shifted = fixed + (places - fixed + offset_by * (used - fixed)) % max(1, number_of - fixed)
        return jnp.zeros((number_of,), jnp.int32).at[sequence[jnp.where(places < fixed, places, shifted)]].set(jnp.asarray(tallies, jnp.int32))

    tallies = jnp.where(number % 4 == 0, named(packed, number // 4), named(ordinary, number - number // 4 - 1))
    mixed = jax.random.permutation(jax.random.fold_in(own, 3), number_of)
    donor, receiver = mixed[0:number_of // 2 * 2:2], mixed[1:number_of // 2 * 2:2]
    room = jnp.minimum(tallies[donor] - 1, bound - tallies[receiver]) // 2
    room = jnp.where((donor == sequence[0]) | (receiver == sequence[0]) | (tallies[receiver] == 0), 0, jnp.maximum(room, 0))
    shifted = jax.random.randint(jax.random.fold_in(own, 4), (number_of // 2,), 0, 1 << 20) % (room + 1)
    tallies = tallies.at[donor].add(-shifted).at[receiver].add(shifted)
    members = jnp.searchsorted(jnp.cumsum(tallies), jnp.arange(rows * top), side="right").astype(jnp.int32)
    table = members.reshape(top, rows).T
    table = table[jax.random.permutation(jax.random.fold_in(own, 1), rows)]
    offset_by = jax.random.randint(jax.random.fold_in(own, 2), (rows, 1), 0, top)
    return jnp.take_along_axis(table, (jnp.arange(top)[None, :] + offset_by) % top, axis=1)


def shares(count, total, reach, skew, full):
    portions = [(1 << 20) // math.isqrt(grade ** skew) + 1 for grade in range(1, count + 1)]
    largest = reach if full else min(reach, max(-(-total // count), total * portions[0] // sum(portions)))
    least = 1 if total - largest >= count - 1 else 0
    holding, surplus = [largest] + [least] * (count - 1), total - largest - least * (count - 1)
    while surplus > 0:
        movable = [i for i in range(1, count) if holding[i] < largest] or [i for i in range(1, count) if holding[i] < reach]
        mass, remaining = sum([portions[i] for i in movable]), surplus
        for i in movable:
            addition = min(reach - holding[i], max(1, remaining * portions[i] // mass), surplus)
            holding[i] = holding[i] + addition
            surplus = surplus - addition
    return np.array(holding)


def normal_values(own_key, extent, scale, most, split=(), kind=jnp.bfloat16):
    gain = steps_of(own_key, extent, split, -0.22, 0.18) if split else 1.0
    entries = jax.random.normal(own_key, extent, jnp.float32) * scale * gain
    return jnp.minimum(jnp.maximum(entries, -most), most).astype(kind)


def setup_inputs(seed: int = 0) -> dict:
    key_list = jax.random.split(jax.random.key(seed), 8)
    tokens = normal_values(key_list[0], (TOKENS, D), 1.0, 6.0, ((0, 8),))
    norm_gain = jnp.clip(1.0 + 0.18 * jax.random.normal(key_list[1], (D,), jnp.float32), 0.1, 1.9)
    expert_ids_keys = jax.random.split(jax.random.fold_in(key_list[2], 1), TOKENS // TOK_DEV)
    expert_ids_turns = jax.random.permutation(jax.random.fold_in(key_list[2], 3), TOKENS // TOK_DEV)
    expert_ids = jax.vmap(lambda own, number: assign_block(jax.random.fold_in(key_list[2], 2), own, number, TOK_DEV, EXPERTS, TOP, CAP, 1))(expert_ids_keys, expert_ids_turns).reshape((TOKENS, TOP))
    route_weight = jnp.clip(0.2 + 0.8 * jax.random.uniform(key_list[3], (TOKENS, TOP), jnp.float32) ** steps_of(key_list[3], (TOKENS, TOP), ((0, 8),), -0.2, 0.2), 0.2, 1.0)
    w_gate = normal_values(key_list[4], (EXPERTS * HALVES, D, HALF_FF), D ** -0.5, 0.125, ((0, 8), (2, 4)))
    w_up = normal_values(key_list[5], (EXPERTS * HALVES, D, HALF_FF), D ** -0.5, 0.125, ((0, 8), (2, 4)))
    w_down = normal_values(key_list[6], (EXPERTS * HALVES, HALF_FF, D), FF ** -0.5, 0.0625, ((0, 8), (1, 4)))
    return {"tokens": tokens, "norm_gain": norm_gain, "expert_ids": expert_ids, "route_weight": route_weight, "w_gate": w_gate, "w_up": w_up, "w_down": w_down}


EPSILON = 1e-05

def layer_normed(tokens, norm_gain):
    values = tokens.astype(jnp.float32)
    center = values - lax.optimization_barrier(jnp.mean(values, axis=-1, keepdims=True))
    spread = lax.optimization_barrier(jnp.mean(center * center, axis=-1, keepdims=True))
    return (center * lax.rsqrt(spread + EPSILON) * norm_gain).astype(jnp.bfloat16)

def slot_numbers(chosen, experts):
    onehot = (chosen[..., None] == jnp.arange(experts, dtype=jnp.int32)).astype(jnp.int32)
    before = jnp.cumsum(onehot, axis=1) - onehot
    return lax.optimization_barrier(jnp.sum(before * onehot, axis=-1)).astype(jnp.int32)

def reference(tokens, norm_gain, expert_ids, route_weight, w_gate, w_up, w_down):
    normed = layer_normed(tokens, norm_gain)
    padded = jnp.concatenate([normed, jnp.zeros((1, D), jnp.bfloat16)], axis=0)
    pair_count = TOK_DEV * TOP
    slots = slot_numbers(expert_ids.reshape(N_EP, pair_count), EXPERTS).reshape(-1)
    flat_expert = expert_ids.reshape(-1).astype(jnp.int32)
    index = jnp.arange(TOKENS * TOP, dtype=jnp.int32)
    source = index // pair_count
    owner = index // TOP
    place = (flat_expert * N_EP + source) * CAP + slots
    table = jnp.full((EXPERTS * N_EP * CAP,), TOKENS, jnp.int32).at[place].set(owner)
    table = table.reshape(EXPERTS, N_EP * CAP)

    def one_expert(expert):
        rows = padded[table[expert]]
        total = jnp.zeros((N_EP * CAP, D), jnp.float32)
        for half in range(HALVES):
            which = expert * HALVES + half
            gate = jnp.dot(rows, w_gate[which], preferred_element_type=jnp.float32)
            up = jnp.dot(rows, w_up[which], preferred_element_type=jnp.float32)
            hidden = (jax.nn.silu(gate) * up).astype(jnp.bfloat16)
            blocks = hidden.reshape(N_EP * CAP, N_TP, BLOCK_H).astype(jnp.float32)
            down = w_down[which].reshape(N_TP, BLOCK_H, D).astype(jnp.float32)
            block_out = jnp.einsum('rnb,nbd->nrd', blocks, down).astype(jnp.bfloat16)
            half_out = lax.optimization_barrier(jnp.sum(block_out.astype(jnp.float32), axis=0)).astype(jnp.bfloat16)
            total = total + half_out.astype(jnp.float32)
        return total
    results = lax.map(one_expert, jnp.arange(EXPERTS, dtype=jnp.int32))
    merged = results.reshape(EXPERTS * N_EP * CAP, D)
    picked = merged[place].reshape(TOKENS, TOP, D)
    return lax.optimization_barrier(jnp.sum(route_weight[:, :, None] * picked, axis=1)).astype(jnp.bfloat16)
```

```python
import functools

import jax
import jax.numpy as jnp
from jax import lax
from jax.experimental import pallas as pl
from jax.experimental.pallas import tpu as pltpu
from jax.sharding import PartitionSpec as P

HALVES = 2
CORES = 2
EPSILON = 1e-05
MESH = pl.DeviceIdType.MESH


def layer_normed(tokens, norm_gain):
    values = tokens.astype(jnp.float32)
    center = values - jnp.mean(values, axis=-1, keepdims=True)
    spread = jnp.mean(center * center, axis=-1, keepdims=True)
    return (center * lax.rsqrt(spread + EPSILON) * norm_gain).astype(jnp.bfloat16)


def slot_numbers(chosen, experts):
    onehot = (chosen[..., None] == jnp.arange(experts, dtype=jnp.int32)).astype(jnp.int32)
    before = jnp.cumsum(onehot, axis=1) - onehot
    return jnp.sum(before * onehot, axis=-1)


def capacity_of(tok_rows, top_count, experts):
    return 2 * min(tok_rows // 2, 5 * tok_rows * top_count // (8 * experts))


def kernel(experts, cap, tokens_ref, gain_ref, ids_ref, weight_ref, wg_hbm, wu_hbm, wd_hbm,
           out_ref, wg, wu, wd, routed, away, part, mate, chip, hop1, turn, hop2, final, back,
           load_sem, zs, zr, xs, xr, ys, yr, fs, fr, ds, dr, ms, mr, h1s, h1r, h2s, h2r, bs, br):
    ep, tp = lax.axis_index("ep"), lax.axis_index("tp")
    z, y = ep // HALVES, ep % HALVES
    x, c = tp // CORES, tp % CORES
    tok_rows, width = tokens_ref.shape
    quarter = out_ref.shape[1]
    bf16, f32 = jnp.bfloat16, jnp.float32

    loads = [
        pltpu.make_async_copy(src.at[0], dst, load_sem.at[i])
        for i, (src, dst) in enumerate(((wg_hbm, wg), (wu_hbm, wu), (wd_hbm, wd)))
    ]
    for load in loads:
        load.start()

    def device(zz, yy, xx, cc):
        return (zz * HALVES + yy, xx * CORES + cc)

    x_peer = device(z, y, 1 - x, c)
    y_peer = device(z, 1 - y, x, c)
    mate_peer = device(z, y, x, 1 - c)
    first = (z * HALVES + (c * (1 - y) + (1 - c) * y), (c * x + (1 - c) * (1 - x)) * CORES + c)
    second = (z * HALVES + (c * y + (1 - c) * (1 - y)), (c * (1 - x) + (1 - c) * x) * CORES + c)

    def z_peer(o):
        return device((z + o) % experts, y, x, c)

    barrier = pltpu.get_barrier_semaphore()
    peers = [x_peer, y_peer, mate_peer] + [z_peer(o) for o in range(1, experts)]
    for peer in peers:
        pl.semaphore_signal(barrier, inc=1, device_id=peer, device_id_type=MESH)

    ids = ids_ref[...]
    one, two = ids[:, 0:1], ids[:, 1:2]
    lane = lax.broadcasted_iota(jnp.int32, (tok_rows, 128), 1)
    expert = (lane + z) % experts
    named = jnp.logical_or(one == expert, two == expert)
    lower = (
        lax.broadcasted_iota(jnp.int32, (tok_rows, tok_rows), 1)
        < lax.broadcasted_iota(jnp.int32, (tok_rows, tok_rows), 0)
    )
    slot = jnp.dot(
        lower.astype(f32).astype(bf16), named.astype(f32).astype(bf16), preferred_element_type=f32
    )
    slot = jnp.where(named, slot, -1.0).astype(jnp.int32)
    places = lax.broadcasted_iota(jnp.int32, (tok_rows, cap), 1)

    def chosen(o):
        return places == slot[:, o:o + 1]

    values = tokens_ref[...].astype(f32)
    mean = jnp.mean(values, axis=-1, keepdims=True)
    center = values - mean
    spread = jnp.mean(center * center, axis=-1, keepdims=True)
    mine = pl.ds(pl.multiple_of(tp * quarter, quarter), quarter)
    own = tokens_ref[:, mine].astype(f32) - mean
    normed = (own * lax.rsqrt(spread + EPSILON) * gain_ref[:, mine]).astype(bf16)

    def outgoing(o):
        return lax.dot_general(
            chosen(o).astype(f32).astype(bf16), normed, (((0,), (0,)), ((), ())),
            preferred_element_type=f32,
        ).astype(bf16)

    def block(d, yy, xx, cc):
        rows = pl.ds(pl.multiple_of(yy * cap, cap), cap)
        columns = pl.ds(pl.multiple_of((xx * CORES + cc) * quarter, quarter), quarter)
        return routed.at[d, rows, columns]

    def send(src, dst, send_sem, recv_sem, peer):
        copy = pltpu.make_async_remote_copy(
            src_ref=src, dst_ref=dst, send_sem=send_sem, recv_sem=recv_sem,
            device_id=peer, device_id_type=MESH,
        )
        copy.start()
        return copy

    order = sorted(range(experts), key=lambda d: min(d, experts - d))
    sent = []
    for o in order:
        if o:
            away[o - 1] = outgoing(o)
    pl.semaphore_wait(barrier, len(peers))
    z_copies = {}
    for o in order:
        if o:
            d = experts - o
            z_copies[d] = send(away.at[o - 1], block(d, y, x, c), zs.at[d], zr.at[d], z_peer(o))
    routed[0, pl.ds(pl.multiple_of(y * cap, cap), cap), mine] = outgoing(0)

    x_copies, y_copies, forwards, pairs, mates = {}, {}, {}, {}, {}

    def launch(d):
        if d:
            z_copies[d].wait_recv()
        b = block(d, y, x, c)
        x_copies[d] = send(b, b, xs.at[d], xr.at[d], x_peer)
        y_copies[d] = send(b, b, ys.at[d], yr.at[d], y_peer)
        pairs[d] = [send(b, b, ds.at[d, 0], dr.at[d, 0], mate_peer)]

    def relay(d):
        x_copies[d].wait_recv()
        y_copies[d].wait_recv()
        b = block(d, c * y + (1 - c) * (1 - y), c * (1 - x) + (1 - c) * x, c)
        forwards[d] = send(b, b, fs.at[d], fr.at[d], first)
        for i, b in ((1, block(d, y, 1 - x, c)), (2, block(d, 1 - y, x, c))):
            pairs[d].append(send(b, b, ds.at[d, i], dr.at[d, i], mate_peer))

    def finish(d):
        forwards[d].wait_recv()
        b = block(d, 1 - y, 1 - x, c)
        pairs[d].append(send(b, b, ds.at[d, 3], dr.at[d, 3], mate_peer))
        for copy in pairs[d]:
            copy.wait_recv()

    def columns_of(xx, cc):
        return pl.ds(pl.multiple_of((xx * CORES + cc) * quarter, quarter), quarter)

    def compute(d):
        rows = routed[d]
        gate = jnp.dot(rows, wg[...], preferred_element_type=f32)
        up = jnp.dot(rows, wu[...], preferred_element_type=f32)
        hidden = (gate / (1.0 + jnp.exp(-gate)) * up).astype(bf16)
        if d == 0:
            loads[2].wait()
        for xx in range(2):
            part[d, 1 - c, xx] = jnp.dot(
                hidden, wd[:, columns_of(xx, 1 - c)], preferred_element_type=f32
            ).astype(bf16)
        mates[d] = send(part.at[d, 1 - c], mate.at[d], ms.at[d], mr.at[d], mate_peer)
        for xx in range(2):
            part[d, c, xx] = jnp.dot(
                hidden, wd[:, columns_of(xx, c)], preferred_element_type=f32
            ).astype(bf16)

    hop1_copies, hop2_copies, back_copies = {}, {}, {}

    def return_first(d):
        mates[d].wait_recv()
        for j in (2, 3, 0, 1):
            low, high = j % 2, j // 2
            x_low, x_high = (1 - x if low else x), (1 - x if high else x)
            y_low, y_high = (1 - y if low else y), (1 - y if high else y)
            xx = c * x_low + (1 - c) * x_high
            yy = c * y_high + (1 - c) * y_low
            rows = pl.ds(pl.multiple_of(yy * cap, cap), cap)
            chip[d, j] = (part[d, c, xx, rows].astype(f32) + mate[d, xx, rows].astype(f32)).astype(bf16)
            if j == 3:
                hop1_copies[d] = send(chip.at[d, pl.ds(2, 2)], hop1.at[d], h1s.at[d], h1r.at[d], first)

    def return_second(d):
        hop1_copies[d].wait_recv()
        turn[d] = (chip[d, 1].astype(f32) + hop1[d, 1].astype(f32)).astype(bf16)
        hop2_copies[d] = send(turn.at[d], hop2.at[d], h2s.at[d], h2r.at[d], second)

    def return_third(d):
        hop2_copies[d].wait_recv()
        total = chip[d, 0].astype(f32) + hop1[d, 0].astype(f32) + hop2[d].astype(f32)
        if d == 0:
            back[0] = total.astype(bf16)
        else:
            final[d] = total.astype(bf16)
            o = experts - d
            back_copies[d] = send(final.at[d], back.at[o], bs.at[o], br.at[o], z_peer(d))

    launch(order[0])
    for k, d in enumerate(order):
        if k + 1 < experts:
            launch(order[k + 1])
        relay(d)
        if k >= 1:
            return_second(order[k - 1])
        finish(d)
        if k == 0:
            loads[0].wait()
            loads[1].wait()
        compute(d)
        return_first(d)
        if k >= 1:
            return_third(order[k - 1])
    return_second(order[-1])
    return_third(order[-1])

    total = jnp.zeros((tok_rows, quarter), f32)
    for o in order:
        if o:
            back_copies[experts - o].wait_recv()
        e = (z + o) % experts
        share = jnp.where(one == e, weight_ref[:, 0:1], 0.0) + jnp.where(two == e, weight_ref[:, 1:2], 0.0)
        mix = jnp.where(chosen(o), share, 0.0)
        high = mix.astype(bf16)
        low = (mix - high.astype(f32)).astype(bf16)
        rows = back[o]
        total += jnp.dot(high, rows, preferred_element_type=f32)
        total += jnp.dot(low, rows, preferred_element_type=f32)
    out_ref[...] = total.astype(bf16)

    for group in (z_copies, x_copies, y_copies, forwards, mates, hop1_copies, hop2_copies, back_copies):
        for d in group:
            group[d].wait_send()
    for d in pairs:
        for copy in pairs[d]:
            copy.wait_send()


def fused_body(tokens, norm_gain, expert_ids, route_weight, w_gate, w_up, w_down):
    tok_rows, width = tokens.shape
    experts = lax.axis_size("ep") // HALVES
    cap = capacity_of(tok_rows, expert_ids.shape[1], experts)
    tp_count = lax.axis_size("tp")
    quarter = width // tp_count
    units = w_gate.shape[2]
    bf16 = jnp.bfloat16
    dma = pltpu.SemaphoreType.DMA
    vmem = pl.BlockSpec(memory_space=pltpu.VMEM)
    hbm = pl.BlockSpec(memory_space=pl.ANY)
    one = dma((experts,))
    return pl.pallas_call(
        functools.partial(kernel, experts, cap),
        out_shape=jax.ShapeDtypeStruct((tok_rows, quarter), bf16),
        in_specs=[vmem, vmem, vmem, vmem, hbm, hbm, hbm],
        out_specs=vmem,
        scratch_shapes=[
            pltpu.VMEM((width, units), bf16),
            pltpu.VMEM((width, units), bf16),
            pltpu.VMEM((units, width), bf16),
            pltpu.VMEM((experts, HALVES * cap, width), bf16),
            pltpu.VMEM((experts - 1, cap, quarter), bf16),
            pltpu.VMEM((experts, CORES, 2, HALVES * cap, quarter), bf16),
            pltpu.VMEM((experts, 2, HALVES * cap, quarter), bf16),
            pltpu.VMEM((experts, 4, cap, quarter), bf16),
            pltpu.VMEM((experts, 2, cap, quarter), bf16),
            pltpu.VMEM((experts, cap, quarter), bf16),
            pltpu.VMEM((experts, cap, quarter), bf16),
            pltpu.VMEM((experts, cap, quarter), bf16),
            pltpu.VMEM((experts, cap, quarter), bf16),
            dma((3,)),
            one, one, one, one, one, one, one, one,
            dma((experts, 4)), dma((experts, 4)),
            one, one, one, one, one, one, one, one,
        ],
        compiler_params=pltpu.CompilerParams(
            collective_id=0, has_side_effects=True, vmem_limit_bytes=60 * 1024 * 1024
        ),
        name="expert_layer",
    )(tokens, norm_gain.reshape(1, -1), expert_ids, route_weight, w_gate, w_up, w_down)


def body(tokens, norm_gain, expert_ids, route_weight, w_gate, w_up, w_down):
    tok_rows, width = tokens.shape
    top_count = expert_ids.shape[1]
    ep_count = lax.axis_size("ep")
    experts = ep_count // HALVES
    capacity = capacity_of(tok_rows, top_count, experts)
    normed = layer_normed(tokens, norm_gain)
    padded = jnp.concatenate([normed, jnp.zeros((1, width), jnp.bfloat16)], axis=0)
    slots = slot_numbers(expert_ids.reshape(1, -1), experts).reshape(-1)
    flat_expert = expert_ids.reshape(-1)
    owner = jnp.arange(tok_rows * top_count, dtype=jnp.int32) // top_count
    place = flat_expert * capacity + slots
    table = jnp.full((experts * capacity,), tok_rows, jnp.int32).at[place].set(owner)
    outgoing = padded[table].reshape(experts, capacity, width)
    columns = width // lax.axis_size("tp")
    portion = lax.dynamic_slice_in_dim(outgoing, lax.axis_index("tp") * columns, columns, 2)
    doubled = jnp.repeat(portion, HALVES, axis=0)
    pieces = lax.all_to_all(doubled, "ep", split_axis=0, concat_axis=0, tiled=True)
    arrived = lax.all_gather(pieces, "tp", axis=2, tiled=True)
    routed = arrived.reshape(-1, width)
    gate = jnp.dot(routed, w_gate[0], preferred_element_type=jnp.float32)
    up = jnp.dot(routed, w_up[0], preferred_element_type=jnp.float32)
    hidden = (jax.nn.silu(gate) * up).astype(jnp.bfloat16)
    partial_value = jnp.dot(hidden, w_down[0], preferred_element_type=jnp.float32)
    reduced = lax.psum_scatter(
        partial_value.astype(jnp.bfloat16), "tp", scatter_dimension=1, tiled=True
    )
    returned = lax.all_to_all(
        reduced.reshape(ep_count, capacity, -1), "ep", split_axis=0, concat_axis=0, tiled=True
    )
    quarter = returned.shape[2]
    summed = returned.reshape(experts, HALVES, capacity, quarter).astype(jnp.float32).sum(axis=1)
    picked = summed.reshape(experts * capacity, quarter)[place].reshape(
        tok_rows, top_count, quarter
    )
    mixed = jnp.sum(route_weight[:, :, None] * picked, axis=1)
    return mixed.astype(jnp.bfloat16)


def choose(*args):
    tok_rows = args[0].shape[0]
    experts = lax.axis_size("ep") // HALVES
    cap = capacity_of(tok_rows, args[2].shape[1], experts)
    if cap % 16 == 0 and lax.axis_size("tp") == 2 * CORES and args[2].shape[1] == 2:
        return fused_body(*args)
    return body(*args)


def solution(mesh):
    return jax.shard_map(
        choose,
        mesh=mesh,
        in_specs=(
            P("ep", None),
            P(),
            P("ep", None),
            P("ep", None),
            P("ep", None, "tp"),
            P("ep", None, "tp"),
            P("ep", "tp", None),
        ),
        out_specs=P("ep", "tp"),
        check_vma=False,
    )
```

```python
import functools

import jax
import jax.numpy as jnp
from jax import lax
from jax.experimental import pallas as pl
from jax.experimental.pallas import tpu as pltpu
from jax.sharding import PartitionSpec as P

HALVES = 2
CORES = 2
EPSILON = 1e-05
MESH = pl.DeviceIdType.MESH


def layer_normed(tokens, norm_gain):
    values = tokens.astype(jnp.float32)
    center = values - jnp.mean(values, axis=-1, keepdims=True)
    spread = jnp.mean(center * center, axis=-1, keepdims=True)
    return (center * lax.rsqrt(spread + EPSILON) * norm_gain).astype(jnp.bfloat16)


def slot_numbers(chosen, experts):
    onehot = (chosen[..., None] == jnp.arange(experts, dtype=jnp.int32)).astype(jnp.int32)
    before = jnp.cumsum(onehot, axis=1) - onehot
    return jnp.sum(before * onehot, axis=-1)


def capacity_of(tok_rows, top_count, experts):
    return 2 * min(tok_rows // 2, 5 * tok_rows * top_count // (8 * experts))


def kernel(experts, cap, tokens_ref, gain_ref, ids_ref, weight_ref, wg_hbm, wu_hbm, wd_hbm,
           out_hbm, wg, wu, wd, out_ref, routed, away, part, mate, chip, hop1, turn, hop2, final, back,
           load_sem, zs, zr, xs, xr, ys, yr, fs, fr, ds, dr, ms, mr, h1s, h1r, h2s, h2r, bs, br):
    ep, tp = lax.axis_index("ep"), lax.axis_index("tp")
    z, y = ep // HALVES, ep % HALVES
    x, c = tp // CORES, tp % CORES
    tok_rows, width = tokens_ref.shape
    quarter = out_ref.shape[1]
    bf16, f32 = jnp.bfloat16, jnp.float32

    loads = [
        pltpu.make_async_copy(src.at[0], dst, load_sem.at[i])
        for i, (src, dst) in enumerate(((wg_hbm, wg), (wu_hbm, wu), (wd_hbm, wd)))
    ]
    for load in loads:
        load.start()

    def device(zz, yy, xx, cc):
        return (zz * HALVES + yy, xx * CORES + cc)

    x_peer = device(z, y, 1 - x, c)
    y_peer = device(z, 1 - y, x, c)
    mate_peer = device(z, y, x, 1 - c)
    first = (z * HALVES + (c * (1 - y) + (1 - c) * y), (c * x + (1 - c) * (1 - x)) * CORES + c)
    second = (z * HALVES + (c * y + (1 - c) * (1 - y)), (c * (1 - x) + (1 - c) * x) * CORES + c)

    def z_peer(o):
        return device((z + o) % experts, y, x, c)

    barrier = pltpu.get_barrier_semaphore()
    peers = [x_peer, y_peer, mate_peer] + [z_peer(o) for o in range(1, experts)]
    for peer in peers:
        pl.semaphore_signal(barrier, inc=1, device_id=peer, device_id_type=MESH)

    ids = jnp.transpose(ids_ref[...])
    one, two = ids[:, 0:1], ids[:, 1:2]
    lane = lax.broadcasted_iota(jnp.int32, (tok_rows, 128), 1)
    expert = (lane + z) % experts
    named = jnp.logical_or(one == expert, two == expert)
    lower = (
        lax.broadcasted_iota(jnp.int32, (tok_rows, tok_rows), 1)
        < lax.broadcasted_iota(jnp.int32, (tok_rows, tok_rows), 0)
    )
    slot = jnp.dot(
        lower.astype(f32).astype(bf16), named.astype(f32).astype(bf16), preferred_element_type=f32
    )
    slot = jnp.where(named, slot, -1.0).astype(jnp.int32)
    places = lax.broadcasted_iota(jnp.int32, (tok_rows, cap), 1)

    def chosen(o):
        return places == slot[:, o:o + 1]

    values = tokens_ref[...].astype(f32)
    mean = jnp.mean(values, axis=-1, keepdims=True)
    center = values - mean
    spread = jnp.mean(center * center, axis=-1, keepdims=True)
    mine = pl.ds(pl.multiple_of(tp * quarter, quarter), quarter)
    own = tokens_ref[:, mine].astype(f32) - mean
    normed = (own * lax.rsqrt(spread + EPSILON) * gain_ref[:, mine]).astype(bf16)

    def outgoing(o):
        return lax.dot_general(
            chosen(o).astype(f32).astype(bf16), normed, (((0,), (0,)), ((), ())),
            preferred_element_type=f32,
        ).astype(bf16)

    def block(d, yy, xx, cc):
        rows = pl.ds(pl.multiple_of(yy * cap, cap), cap)
        columns = pl.ds(pl.multiple_of((xx * CORES + cc) * quarter, quarter), quarter)
        return routed.at[d, rows, columns]

    def send(src, dst, send_sem, recv_sem, peer):
        copy = pltpu.make_async_remote_copy(
            src_ref=src, dst_ref=dst, send_sem=send_sem, recv_sem=recv_sem,
            device_id=peer, device_id_type=MESH,
        )
        copy.start()
        return copy

    order = [0] + sorted(range(1, experts), key=lambda d: -min(d, experts - d))
    turns = order
    for o in order:
        if o:
            away[o - 1] = outgoing(o)
    pl.semaphore_wait(barrier, len(peers))
    z_copies = {}
    for o in order:
        if o:
            d = experts - o
            z_copies[d] = send(away.at[o - 1], block(d, y, x, c), zs.at[d], zr.at[d], z_peer(o))
    routed[0, pl.ds(pl.multiple_of(y * cap, cap), cap), mine] = outgoing(0)

    x_copies, y_copies, forwards, pairs, mates = {}, {}, {}, {}, {}

    def launch(d):
        if d:
            z_copies[d].wait_recv()
        b = block(d, y, x, c)
        x_copies[d] = send(b, b, xs.at[d], xr.at[d], x_peer)
        y_copies[d] = send(b, b, ys.at[d], yr.at[d], y_peer)
        pairs[d] = [send(b, b, ds.at[d, 0], dr.at[d, 0], mate_peer)]

    def relay(d):
        x_copies[d].wait_recv()
        y_copies[d].wait_recv()
        b = block(d, c * y + (1 - c) * (1 - y), c * (1 - x) + (1 - c) * x, c)
        forwards[d] = send(b, b, fs.at[d], fr.at[d], first)
        for i, b in ((1, block(d, y, 1 - x, c)), (2, block(d, 1 - y, x, c))):
            pairs[d].append(send(b, b, ds.at[d, i], dr.at[d, i], mate_peer))

    def finish(d):
        forwards[d].wait_recv()
        b = block(d, 1 - y, 1 - x, c)
        pairs[d].append(send(b, b, ds.at[d, 3], dr.at[d, 3], mate_peer))
        for copy in pairs[d]:
            copy.wait_recv()

    def columns_of(xx, cc):
        return pl.ds(pl.multiple_of((xx * CORES + cc) * quarter, quarter), quarter)

    def compute(d, early, between):
        rows = routed[d]
        gate = jnp.dot(rows, wg[...], preferred_element_type=f32)
        up = jnp.dot(rows, wu[...], preferred_element_type=f32)
        hidden = (gate / (1.0 + jnp.exp(-gate)) * up).astype(bf16)
        between()
        if early:
            loads[2].wait()
        for xx in range(2):
            part[d, 1 - c, xx] = jnp.dot(
                hidden, wd[:, columns_of(xx, 1 - c)], preferred_element_type=f32
            ).astype(bf16)
        mates[d] = send(part.at[d, 1 - c], mate.at[d], ms.at[d], mr.at[d], mate_peer)
        for xx in range(2):
            part[d, c, xx] = jnp.dot(
                hidden, wd[:, columns_of(xx, c)], preferred_element_type=f32
            ).astype(bf16)

    hop1_copies, hop2_copies, back_copies = {}, {}, {}

    def return_first(d):
        mates[d].wait_recv()
        for j in (2, 3, 0, 1):
            low, high = j % 2, j // 2
            x_low, x_high = (1 - x if low else x), (1 - x if high else x)
            y_low, y_high = (1 - y if low else y), (1 - y if high else y)
            xx = c * x_low + (1 - c) * x_high
            yy = c * y_high + (1 - c) * y_low
            rows = pl.ds(pl.multiple_of(yy * cap, cap), cap)
            chip[d, j] = (part[d, c, xx, rows].astype(f32) + mate[d, xx, rows].astype(f32)).astype(bf16)
            if j == 3:
                hop1_copies[d] = send(chip.at[d, pl.ds(2, 2)], hop1.at[d], h1s.at[d], h1r.at[d], first)

    def return_second(d):
        hop1_copies[d].wait_recv()
        turn[d] = (chip[d, 1].astype(f32) + hop1[d, 1].astype(f32)).astype(bf16)
        hop2_copies[d] = send(turn.at[d], hop2.at[d], h2s.at[d], h2r.at[d], second)

    def return_third(d):
        hop2_copies[d].wait_recv()
        total = chip[d, 0].astype(f32) + hop1[d, 0].astype(f32) + hop2[d].astype(f32)
        if d == 0:
            back[0] = total.astype(bf16)
        else:
            final[d] = total.astype(bf16)
            o = experts - d
            back_copies[d] = send(final.at[d], back.at[o], bs.at[o], br.at[o], z_peer(d))

    look = 2
    for k in range(look):
        launch(order[k])
    for k in range(look - 1):
        relay(order[k])

    def ahead(k):
        if k + look < experts:
            launch(order[k + look])
        if k + look - 1 < experts:
            relay(order[k + look - 1])

    for k, d in enumerate(turns):
        def between(k=k):
            pass
            if k >= 1:
                return_second(turns[k - 1])

        ahead(k)
        finish(d)
        if k == 0:
            loads[0].wait()
            loads[1].wait()
        compute(d, k == 0, between)
        return_first(d)
        if k >= 2:
            return_third(turns[k - 2])
    return_second(turns[-1])
    return_third(turns[-2])
    return_third(turns[-1])

    total = jnp.zeros((tok_rows, quarter), f32)
    route = jnp.transpose(weight_ref[...])
    for o in order:
        if o:
            back_copies[experts - o].wait_recv()
        e = (z + o) % experts
        share = jnp.where(one == e, route[:, 0:1], 0.0) + jnp.where(two == e, route[:, 1:2], 0.0)
        mix = jnp.where(chosen(o), share, 0.0)
        high = mix.astype(bf16)
        low = (mix - high.astype(f32)).astype(bf16)
        rows = back[o]
        total += jnp.dot(high, rows, preferred_element_type=f32)
        total += jnp.dot(low, rows, preferred_element_type=f32)
    out_ref[...] = total.astype(bf16)
    store = pltpu.make_async_copy(out_ref, out_hbm, load_sem.at[3])
    store.start()

    for group in (z_copies, x_copies, y_copies, forwards, mates, hop1_copies, hop2_copies, back_copies):
        for d in group:
            group[d].wait_send()
    for d in pairs:
        for copy in pairs[d]:
            copy.wait_send()
    store.wait()


def fused_body(tokens, norm_gain, expert_ids, route_weight, w_gate, w_up, w_down):
    tok_rows, width = tokens.shape
    experts = lax.axis_size("ep") // HALVES
    cap = capacity_of(tok_rows, expert_ids.shape[1], experts)
    tp_count = lax.axis_size("tp")
    quarter = width // tp_count
    units = w_gate.shape[2]
    bf16 = jnp.bfloat16
    dma = pltpu.SemaphoreType.DMA
    vmem = pl.BlockSpec(memory_space=pltpu.VMEM)
    hbm = pl.BlockSpec(memory_space=pl.ANY)
    one = dma((experts,))
    return pl.pallas_call(
        functools.partial(kernel, experts, cap),
        out_shape=jax.ShapeDtypeStruct((tok_rows, quarter), bf16),
        in_specs=[vmem, vmem, vmem, vmem, hbm, hbm, hbm],
        out_specs=hbm,
        scratch_shapes=[
            pltpu.VMEM((width, units), bf16),
            pltpu.VMEM((width, units), bf16),
            pltpu.VMEM((units, width), bf16),
            pltpu.VMEM((tok_rows, quarter), bf16),
            pltpu.VMEM((experts, HALVES * cap, width), bf16),
            pltpu.VMEM((experts - 1, cap, quarter), bf16),
            pltpu.VMEM((experts, CORES, 2, HALVES * cap, quarter), bf16),
            pltpu.VMEM((experts, 2, HALVES * cap, quarter), bf16),
            pltpu.VMEM((experts, 4, cap, quarter), bf16),
            pltpu.VMEM((experts, 2, cap, quarter), bf16),
            pltpu.VMEM((experts, cap, quarter), bf16),
            pltpu.VMEM((experts, cap, quarter), bf16),
            pltpu.VMEM((experts, cap, quarter), bf16),
            pltpu.VMEM((experts, cap, quarter), bf16),
            dma((4,)),
            one, one, one, one, one, one, one, one,
            dma((experts, 4)), dma((experts, 4)),
            one, one, one, one, one, one, one, one,
        ],
        compiler_params=pltpu.CompilerParams(
            collective_id=0, has_side_effects=True, vmem_limit_bytes=60 * 1024 * 1024
        ),
        name="expert_layer",
    )(tokens, norm_gain.reshape(1, -1), expert_ids.T, route_weight.T, w_gate, w_up, w_down)


def body(tokens, norm_gain, expert_ids, route_weight, w_gate, w_up, w_down):
    tok_rows, width = tokens.shape
    top_count = expert_ids.shape[1]
    ep_count = lax.axis_size("ep")
    experts = ep_count // HALVES
    capacity = capacity_of(tok_rows, top_count, experts)
    normed = layer_normed(tokens, norm_gain)
    padded = jnp.concatenate([normed, jnp.zeros((1, width), jnp.bfloat16)], axis=0)
    slots = slot_numbers(expert_ids.reshape(1, -1), experts).reshape(-1)
    flat_expert = expert_ids.reshape(-1)
    owner = jnp.arange(tok_rows * top_count, dtype=jnp.int32) // top_count
    place = flat_expert * capacity + slots
    table = jnp.full((experts * capacity,), tok_rows, jnp.int32).at[place].set(owner)
    outgoing = padded[table].reshape(experts, capacity, width)
    columns = width // lax.axis_size("tp")
    portion = lax.dynamic_slice_in_dim(outgoing, lax.axis_index("tp") * columns, columns, 2)
    doubled = jnp.repeat(portion, HALVES, axis=0)
    pieces = lax.all_to_all(doubled, "ep", split_axis=0, concat_axis=0, tiled=True)
    arrived = lax.all_gather(pieces, "tp", axis=2, tiled=True)
    routed = arrived.reshape(-1, width)
    gate = jnp.dot(routed, w_gate[0], preferred_element_type=jnp.float32)
    up = jnp.dot(routed, w_up[0], preferred_element_type=jnp.float32)
    hidden = (jax.nn.silu(gate) * up).astype(jnp.bfloat16)
    partial_value = jnp.dot(hidden, w_down[0], preferred_element_type=jnp.float32)
    reduced = lax.psum_scatter(
        partial_value.astype(jnp.bfloat16), "tp", scatter_dimension=1, tiled=True
    )
    returned = lax.all_to_all(
        reduced.reshape(ep_count, capacity, -1), "ep", split_axis=0, concat_axis=0, tiled=True
    )
    quarter = returned.shape[2]
    summed = returned.reshape(experts, HALVES, capacity, quarter).astype(jnp.float32).sum(axis=1)
    picked = summed.reshape(experts * capacity, quarter)[place].reshape(
        tok_rows, top_count, quarter
    )
    mixed = jnp.sum(route_weight[:, :, None] * picked, axis=1)
    return mixed.astype(jnp.bfloat16)


def choose(*args):
    tok_rows = args[0].shape[0]
    experts = lax.axis_size("ep") // HALVES
    cap = capacity_of(tok_rows, args[2].shape[1], experts)
    if cap % 16 == 0 and lax.axis_size("tp") == 2 * CORES and args[2].shape[1] == 2:
        return fused_body(*args)
    return body(*args)


def solution(mesh):
    return jax.shard_map(
        choose,
        mesh=mesh,
        in_specs=(
            P("ep", None),
            P(),
            P("ep", None),
            P("ep", None),
            P("ep", None, "tp"),
            P("ep", None, "tp"),
            P("ep", "tp", None),
        ),
        out_specs=P("ep", "tp"),
        check_vma=False,
    )
```
